768 devices in a mesh: ep: 24 (over z, core), tp: 32 (over y, x).
Axes of the slice: x: 4, y: 8, z: 12, core: 2. Of those that a mesh axis runs over, the one named last changes fastest.
Arguments:
- tokens: bfloat16 [4032, 2048], P('ep', 'tp'), may hold values from -540 to 540
- norm_gain: float32 [2048], P('tp'), may hold values from 0.1 to 1.9
- chosen: int32 [24, 504], P('ep'), may hold values from 0 to 4031, as said below
- affinity: float32 [24, 504], P('ep'), may hold values from 0.1 to 1
- w_gate: bfloat16 [24, 2048, 8192], P('ep', None, 'tp'), may hold values from -0.125 to 0.125
- w_up: bfloat16 [24, 2048, 8192], P('ep', None, 'tp'), may hold values from -0.125 to 0.125
- w_down: bfloat16 [24, 8192, 2048], P('ep', 'tp'), may hold values from -0.0625 to 0.0625
Outputs:
- expert_mix: bfloat16 [4032, 2048], P('ep', 'tp')
The draws below stay inside these ranges and needn't reach their ends.
Inputs may be any that keep to these rules, and one draw needn't show every extreme that they name: `chosen`: each expert's 504 token numbers are distinct. Among one expert's choices at most 42 are tokens of one index of ep, and that bound is reached in every draw.
All inputs are finite; a program needn't handle non-finite values.
Results may differ from the reference program's by a relative error of at most 0.025.
Values may be sent and summed in bfloat16 or wider, within the bound.
No kernel may reach another device: no remote copies, remote signals or barrier semaphores. Data moves between devices by JAX's collectives and lax.ppermute only.
A program may use at most 32 MiB of HBM per device.

```python
import math
import jax
import jax.numpy as jnp
from jax import lax

D = 2048
FF = 8192
TOK_DEV = 168
TOKENS = 4032
EXPERTS = 24
CHOSEN = 504
MOST = 42
N_TP = 32


def draw_tokens(key, part):
    key_noise, key_cols, key_rows = jax.random.split(key, 3)
    col_scale = 6.0 ** (jnp.arange(D, dtype=jnp.float32) / (D - 1))
    col_scale = col_scale * jax.random.uniform(key_cols, (D,), jnp.float32, 0.5, 1.5)
    row_scale = jnp.exp(jax.random.uniform(key_rows, (TOKENS, 1), jnp.float32, 0.0, math.log(10.0)))
    noise = jnp.clip(jax.random.normal(key_noise, (TOKENS, D), jnp.float32), -6.0, 6.0)
    return (noise * col_scale[None, :] * row_scale).astype(jnp.bfloat16)


def draw_chosen(key, part):

    def pick_expert(expert):
        expert_key = jax.random.fold_in(key, expert)
        key_raw, key_full = jax.random.split(expert_key, 2)
        raw_score = jax.random.randint(key_raw, (EXPERTS, TOK_DEV), 0, 32768)
        local_id = jnp.arange(TOK_DEV, dtype=jnp.int32)[None, :]
        source = jnp.arange(EXPERTS, dtype=jnp.int32)[:, None]
        global_id = source * TOK_DEV + local_id
        keyed_score = raw_score * TOK_DEV + local_id
        ranked = jnp.argsort(jnp.argsort(-keyed_score, axis=1), axis=1)
        allowed = ranked < MOST
        full_source = jax.random.randint(key_full, (), 0, EXPERTS)
        before = (expert + EXPERTS - 1) % EXPERTS
        across = (expert + EXPERTS // 2) % EXPERTS
        extra_score = jnp.where(source == full_source, 2, 0)
        extra_score = extra_score + jnp.where(((source == before) | (source == across)) & (ranked == 0), 4, 0)
        priority = allowed.astype(jnp.int32) * (extra_score + 1) * (1 << 27) + raw_score * TOKENS + global_id
        return lax.top_k(priority.reshape(-1), CHOSEN)[1].astype(jnp.int32)
    from_experts = jax.vmap(pick_expert)(jnp.arange(EXPERTS, dtype=jnp.int32))
    return from_experts.astype(jnp.int32)


def levels(rng, dims, cuts, least, high):
    factor_of, own = 1.0, jax.random.fold_in(rng, 6)
    for position, shards_of in cuts:
        draws = jnp.exp(jax.random.uniform(jax.random.fold_in(own, position), (shards_of,), jnp.float32, least / len(cuts), high / len(cuts)))
        factor_of = factor_of * jnp.repeat(draws, dims[position] // shards_of).reshape([-1 if axis == position else 1 for axis in range(len(dims))])
    return factor_of


def bell_draw(rng, shape, deviation, reach, shards=(), held_as=jnp.bfloat16):
    drawn = deviation * jax.random.normal(rng, shape, jnp.float32)
    if shards:
        drawn = drawn * levels(rng, shape, shards, -0.22, 0.18)
    return jnp.clip(drawn, -reach, reach).astype(held_as)


def setup_inputs(seed: int = 0) -> dict:
    arg_keys = jax.random.split(jax.random.key(seed), 8)
    return {
        "tokens": draw_tokens(jax.random.fold_in(arg_keys[7], 71), 0),
        "norm_gain": jnp.clip(1.0 + 0.18 * jax.random.normal(arg_keys[1], (D,), jnp.float32), 0.1, 1.9),
        "chosen": draw_chosen(jax.random.fold_in(arg_keys[7], 71), 0),
        "affinity": jnp.clip(jnp.exp(math.log(1.0) - 2.3025851 * jax.random.uniform(arg_keys[3], (EXPERTS, CHOSEN), jnp.float32) ** levels(arg_keys[3], (EXPERTS, CHOSEN), ((0, 24),), -0.2, 0.2)), 0.1, 1.0),
        "w_gate": bell_draw(arg_keys[4], (EXPERTS, D, FF), D ** -0.5, 0.125, ((0, 24), (2, 32))),
        "w_up": bell_draw(arg_keys[5], (EXPERTS, D, FF), D ** -0.5, 0.125, ((0, 24), (2, 32))),
        "w_down": bell_draw(arg_keys[6], (EXPERTS, FF, D), FF ** -0.5, 0.0625, ((0, 24), (1, 32))),
    }


EPS = 1e-06

def reference(tokens, norm_gain, chosen, affinity, w_gate, w_up, w_down):
    floats = tokens.astype(jnp.float32)
    mean_square = lax.optimization_barrier(jnp.mean(floats * floats, axis=1))
    normed = (floats * lax.rsqrt(mean_square + EPS)[:, None] * norm_gain[None, :]).astype(jnp.bfloat16)

    def single(packed):
        index_row, weight_row, gate_weights, up_weights, down_weights = packed
        picked = normed[index_row]
        gate = jnp.dot(picked, gate_weights, preferred_element_type=jnp.float32)
        upward = jnp.dot(picked, up_weights, preferred_element_type=jnp.float32)
        hidden = (jax.nn.silu(gate) * upward).astype(jnp.bfloat16)
        blocks = hidden.reshape(hidden.shape[0], N_TP, FF // N_TP).astype(jnp.float32)
        down_blocks = down_weights.reshape(N_TP, FF // N_TP, D).astype(jnp.float32)
        partial_value = jnp.einsum('cnf,nfd->ncd', blocks, down_blocks).astype(jnp.bfloat16)
        partial_value = lax.optimization_barrier(partial_value)
        summed = lax.optimization_barrier(jnp.sum(partial_value.astype(jnp.float32), axis=0))
        return (summed * weight_row[:, None]).astype(jnp.bfloat16)
    outputs = lax.map(single, (chosen, affinity, w_gate, w_up, w_down))
    total = jnp.zeros((TOKENS, D), jnp.float32)
    total = total.at[chosen.reshape(-1)].add(outputs.reshape(-1, D).astype(jnp.float32))
    return total.astype(jnp.bfloat16)
```

```python
import functools

import jax
import jax.numpy as jnp
from jax import lax
from jax.experimental import pallas as pl
from jax.experimental.pallas import tpu as pltpu
from jax.sharding import Mesh, PartitionSpec as P


EPS = 1e-06
SLOTS = 512
VMEM = pl.BlockSpec(memory_space=pltpu.VMEM)
SMEM = pl.BlockSpec(memory_space=pltpu.SMEM)
BF16 = jnp.bfloat16
F32 = jnp.float32
PLANE = ("core", "y", "x")


def call(kernel, outs, args, specs=None, scratch=(), flops=0, vmem=16):
    return pl.pallas_call(
        kernel,
        out_shape=outs,
        in_specs=specs or [VMEM] * len(args),
        out_specs=jax.tree.map(lambda _: VMEM, outs),
        scratch_shapes=list(scratch),
        compiler_params=pltpu.CompilerParams(vmem_limit_bytes=vmem * 1024 * 1024),
        cost_estimate=pl.CostEstimate(flops=flops, bytes_accessed=0, transcendentals=0),
    )(*args)


def place(core, y, x, ny, nx):
    return ((y + core) % ny) * nx + (x + core) % nx


def tiles(ny, nx):
    near, far = [], []
    for c in range(2):
        base = c * ny * nx

        def at(Y, X, b, a, c=c, base=base):
            return base + place(c, 2 * Y + b, 2 * X + a, ny, nx)

        corners = [(b, a) for b in range(2) for a in range(2)]
        cells = [(Y, X) for Y in range(ny // 2) for X in range(nx // 2)]
        near += [[at(Y, X, b, a) for b, a in corners] for Y, X in cells]
        far += [[at(Y, X, b, a) for Y, X in cells] for b, a in corners]
    return near, far


def to_all(array, axis, groups=None):
    n = len(groups[0]) if groups else lax.axis_size(axis)
    return lax.all_to_all(
        jnp.broadcast_to(array[None], (n, *array.shape)),
        axis,
        0,
        0,
        axis_index_groups=groups,
        tiled=True,
    )


def hot(ids, base, rows):
    row = lax.broadcasted_iota(jnp.int32, (rows, ids.shape[1]), 0)
    return jnp.where(row == ids - base, 1.0, 0.0).astype(BF16)


def pick_kernel(core_ref, gathered, own_ref, sib_ref, gain, mine, other):
    blocks, _, rows = gathered.shape
    core = core_ref[0]
    acc = jnp.zeros(mine.shape, F32)
    acc2 = jnp.zeros(mine.shape, F32)
    for b in range(blocks):
        base = (2 * b + core) * rows
        acc += jnp.dot(gathered[b], hot(own_ref[...], base, rows), preferred_element_type=F32)
        acc2 += jnp.dot(gathered[b], hot(sib_ref[...], base, rows), preferred_element_type=F32)
    high = gain[...].astype(BF16)
    rest = gain[...] - high.astype(F32)
    middle = rest.astype(BF16)
    low = (rest - middle.astype(F32)).astype(BF16)
    lane = lax.broadcasted_iota(jnp.int32, mine.shape, 1)
    first = SLOTS - 8
    acc = jnp.where(lane == first, high.astype(F32), acc)
    acc = jnp.where(lane == first + 1, middle.astype(F32), acc)
    acc = jnp.where(lane == first + 2, low.astype(F32), acc)
    mine[...] = acc.astype(BF16)
    other[...] = acc2.astype(BF16)


def block_of(core, corner, cell, ny, nx):
    Y, X = cell // (nx // 2), cell % (nx // 2)
    b, a = corner // 2, corner % 2
    return place(core, 2 * Y + b, 2 * X + a, ny, nx)


def turn_kernel(ny, nx, core_ref, gate_ref, up_ref, out):
    _, _, hid = gate_ref.shape
    cells = ny * nx // 4
    for s in range(4):
        for half, ref in enumerate((gate_ref, up_ref)):
            pieces = [ref[block_of(core_ref[0], s, g, ny, nx)] for g in range(cells)]
            rows = jnp.concatenate(pieces, axis=0)
            out[s, half * hid : (half + 1) * hid] = rows.T


def turn_down_kernel(ny, nx, core_ref, down_ref, out, turned):
    corners, cells, part, hid = out.shape
    for y in range(ny):
        rows = down_ref[:, y * nx * part : (y + 1) * nx * part].T
        turned[y * nx : (y + 1) * nx] = rows.reshape(nx, part, hid)
    for s in range(corners):
        for g in range(cells):
            out[s, g] = turned[block_of(core_ref[0], s, g, ny, nx)]


def hidden_kernel(x_ref, w_ref, out, normed):
    corners, depth, slots = x_ref.shape
    hid = out.shape[0]
    width = corners * depth
    square = jnp.zeros((1, slots), F32)
    for s in range(corners):
        v = x_ref[s].astype(F32)
        square += jnp.sum(v * v, axis=0, keepdims=True)
    scale = lax.rsqrt(square / width + EPS)
    acc = jnp.zeros((2 * hid, slots), F32)
    for s in range(corners):
        v = x_ref[s]
        parts = v[:, slots - 128 :].astype(F32)
        lane = lax.broadcasted_iota(jnp.int32, parts.shape, 1)
        keep = (lane >= 120) & (lane < 123)
        gain = jnp.sum(jnp.where(keep, parts, 0.0), axis=1, keepdims=True)
        normed[...] = (v.astype(F32) * scale * gain).astype(BF16)
        acc += jnp.dot(w_ref[s], normed[...], preferred_element_type=F32)
    gate, up = acc[:hid], acc[hid:]
    out[...] = (gate / (1.0 + jnp.exp(-gate)) * up).astype(BF16)


def down_kernel(corner_ref, hidden, w0, w1, w2, w3, out):
    me = corner_ref[0]
    acc = jnp.zeros(out.shape, F32)
    for flip, w in enumerate((w0, w1, w2, w3)):
        acc += jnp.dot(w[...], hidden[me ^ flip], preferred_element_type=F32)
    out[...] = acc.astype(BF16)


def spread_kernel(core_ref, mine, other, own_ref, sib_ref, out):
    blocks, _, rows = out.shape
    core = core_ref[0]
    dims = (((1,), (1,)), ((), ()))
    for b in range(blocks):
        base = (2 * b + core) * rows
        total = lax.dot_general(
            mine[...], hot(own_ref[...], base, rows), dims, preferred_element_type=F32
        )
        total += lax.dot_general(
            other[...], hot(sib_ref[...], base, rows), dims, preferred_element_type=F32
        )
        out[b] = total.astype(BF16)


def local(tokens, norm_gain, chosen, affinity, w_gate, w_up, w_down):
    tok_dev, part = tokens.shape
    nz, ny, nx = lax.axis_size("z"), lax.axis_size("y"), lax.axis_size("x")
    width, hid = w_gate.shape[1:]
    tp, cells = ny * nx, ny * nx // 4
    near, far = tiles(ny, nx)
    count = chosen.shape[1]
    swap = [(0, 1), (1, 0)]
    core_index = lax.axis_index("core").astype(jnp.int32)
    y_index = lax.axis_index("y").astype(jnp.int32)
    x_index = lax.axis_index("x").astype(jnp.int32)
    corner_index = ((y_index + core_index) & 1) * 2 + ((x_index + core_index) & 1)
    core, corner = core_index.reshape(1), corner_index.reshape(1)

    gathered = to_all(tokens.T, "z")

    own_ids = jnp.pad(chosen, ((0, 0), (0, SLOTS - count)), constant_values=-1)
    sib_ids = lax.ppermute(own_ids, "core", swap)
    down_blocks = call(
        functools.partial(turn_down_kernel, ny, nx),
        jax.ShapeDtypeStruct((4, cells, part, hid), BF16),
        (core, w_down[0]),
        [SMEM, VMEM],
        [pltpu.VMEM((tp, part, hid), BF16)],
        flops=1 << 30,
    ).reshape(4, cells * part, hid)
    downs = [lax.dynamic_index_in_dim(down_blocks, corner_index, 0, False)]
    for flip in range(1, 4):
        block = lax.dynamic_index_in_dim(down_blocks, corner_index ^ flip, 0, False)
        pairs = [(g[s], g[s ^ flip]) for g in near for s in range(4)]
        downs.append(lax.ppermute(block, PLANE, pairs))
    turned = call(
        functools.partial(turn_kernel, ny, nx),
        jax.ShapeDtypeStruct((4, 2 * hid, cells * part), BF16),
        (core, w_gate[0].reshape(tp, part, hid), w_up[0].reshape(tp, part, hid)),
        [SMEM, VMEM, VMEM],
        flops=1 << 30,
    )
    gathered, downs, turned = lax.optimization_barrier((gathered, downs, turned))

    slots = jax.ShapeDtypeStruct((part, SLOTS), BF16)
    own, other = call(
        pick_kernel,
        [slots, slots],
        (core, gathered, own_ids, sib_ids, norm_gain[:, None]),
        [SMEM] + [VMEM] * 4,
        flops=4 * part * nz * tok_dev * SLOTS,
    )
    picked = own + lax.ppermute(other, "core", swap)

    column = to_all(picked, PLANE, far).reshape(cells * part, SLOTS)
    full = to_all(column, PLANE, near)
    hidden = call(
        hidden_kernel,
        jax.ShapeDtypeStruct((hid, SLOTS), BF16),
        (full, turned),
        scratch=[pltpu.VMEM((cells * part, SLOTS), BF16)],
        flops=4 * width * hid * SLOTS,
    )
    tile_hidden = to_all(hidden, PLANE, near)
    partial = call(
        down_kernel,
        jax.ShapeDtypeStruct((cells * part, SLOTS), BF16),
        (corner, tile_hidden, *downs),
        [SMEM] + [VMEM] * 5,
        flops=2 * width * hid * SLOTS,
    )
    arrived = lax.all_to_all(
        partial.reshape(cells, part, SLOTS), PLANE, 0, 0, axis_index_groups=far, tiled=True
    )
    weight = jnp.pad(affinity, ((0, 0), (0, SLOTS - count)))
    weighted = (jnp.sum(arrived.astype(F32), axis=0) * weight).astype(BF16)
    weighted_other = lax.ppermute(weighted, "core", swap)
    dense = call(
        spread_kernel,
        jax.ShapeDtypeStruct((nz, part, tok_dev), BF16),
        (core, weighted, weighted_other, own_ids, sib_ids),
        [SMEM] + [VMEM] * 4,
        flops=4 * part * nz * tok_dev * SLOTS,
    )
    back = lax.all_to_all(dense, "z", 0, 0, tiled=True)
    return jnp.sum(back.astype(F32), axis=0).astype(BF16).T


def solution(mesh):
    nz, ny, nx = 12, 8, 4
    fine = Mesh(mesh.devices.reshape(nz, 2, ny, nx), ("z", "core", "y", "x"))
    ep, tp = ("z", "core"), ("y", "x")
    in_specs = (
        P(ep, tp),
        P(tp),
        P(ep, None),
        P(ep, None),
        P(ep, None, tp),
        P(ep, None, tp),
        P(ep, tp, None),
    )

    return jax.shard_map(local, mesh=fine, in_specs=in_specs, out_specs=P(ep, tp), check_vma=False)
```

```python
import functools

import jax
import jax.numpy as jnp
from jax import lax
from jax.experimental import pallas as pl
from jax.experimental.pallas import tpu as pltpu
from jax.sharding import Mesh, PartitionSpec as P


EPS = 1e-06
SLOTS = 512
HALF = 88
SIDE = 24
VMEM = pl.BlockSpec(memory_space=pltpu.VMEM)
SMEM = pl.BlockSpec(memory_space=pltpu.SMEM)
BF16 = jnp.bfloat16
F32 = jnp.float32
PLANE = ("core", "y", "x")


def call(kernel, outs, args, specs=None, scratch=(), flops=0, vmem=16):
    return pl.pallas_call(
        kernel,
        out_shape=outs,
        in_specs=specs or [VMEM] * len(args),
        out_specs=jax.tree.map(lambda _: VMEM, outs),
        scratch_shapes=list(scratch),
        compiler_params=pltpu.CompilerParams(vmem_limit_bytes=vmem * 1024 * 1024),
        cost_estimate=pl.CostEstimate(flops=flops, bytes_accessed=0, transcendentals=0),
    )(*args)


def place(core, y, x, ny, nx):
    return ((y + core) % ny) * nx + (x + core) % nx


def tiles(ny, nx):
    near, far = [], []
    for c in range(2):
        base = c * ny * nx

        def at(Y, X, b, a, c=c, base=base):
            return base + place(c, 2 * Y + b, 2 * X + a, ny, nx)

        corners = [(b, a) for b in range(2) for a in range(2)]
        cells = [(Y, X) for Y in range(ny // 2) for X in range(nx // 2)]
        near += [[at(Y, X, b, a) for b, a in corners] for Y, X in cells]
        far += [[at(Y, X, b, a) for Y, X in cells] for b, a in corners]
    return near, far


def hot(ids, base, rows):
    row = lax.broadcasted_iota(jnp.int32, (rows, ids.shape[1]), 0)
    return jnp.where(row == ids - base, 1.0, 0.0).astype(BF16)


def pack_kernel(tokens, chosen, out, ids):
    copies, part = out.shape[0], tokens.shape[0]
    ids[...] = jnp.full(ids.shape, 4095, jnp.int32)
    ids[:, : chosen.shape[1]] = chosen[...]
    turned = tokens[...].astype(F32).T
    rest = turned.shape[0] - HALF
    upper = jnp.concatenate([turned[HALF:], jnp.zeros((HALF - rest, part), F32)], axis=0)
    rows = jnp.concatenate([turned[:HALF], upper], axis=1)
    high = (ids[...] >> 6).astype(F32)
    low = (ids[...] & 63).astype(F32)
    lists = [v[:, k : k + 128] for v in (high, low) for k in range(0, SLOTS, 128)]
    body = jnp.concatenate([rows, *lists], axis=0).astype(BF16)
    for k in range(copies):
        out[k] = body


def send_hot_kernel(tok_dev, ids, low, high):
    side = ids.shape[1]
    token = ids[...].astype(F32)
    owner = jnp.floor((token + 0.5) * (1.0 / tok_dev))
    column = jnp.broadcast_to(token, (128, side)).T[:, :1]
    column_owner = jnp.broadcast_to(owner, (128, side)).T[:, :1]
    before = (column < token) & (column_owner == owner)
    rank = jnp.sum(jnp.where(before, 1.0, 0.0), axis=0, keepdims=True)
    code = (owner * (2.0 * SIDE) + rank).astype(jnp.int32)
    row = lax.broadcasted_iota(jnp.int32, (SIDE, side), 0)
    for o in range(low.shape[0]):
        low[o] = jnp.where(code == row + 2 * SIDE * o, 1.0, 0.0).astype(BF16)
        high[o] = jnp.where(code == row + 2 * SIDE * o + SIDE, 1.0, 0.0).astype(BF16)


def pick(tok_dev, core, gathered, ids, part):
    dims = (((0,), (0,)), ((), ()))
    acc = jnp.zeros((part, SLOTS), F32)
    for b in range(gathered.shape[0]):
        for half in range(2):
            base = (2 * b + core) * tok_dev + half * HALF
            rows = gathered[b, :HALF, half * part : (half + 1) * part]
            acc += lax.dot_general(rows, hot(ids, base, HALF), dims, preferred_element_type=F32)
    return acc


def pick_kernel(tok_dev, core_ref, gathered, ids, gain, mine):
    part = gain.shape[1]
    acc = pick(tok_dev, core_ref[0], gathered, ids[...], part)
    square = (part, part)
    same = lax.broadcasted_iota(jnp.int32, square, 0) == lax.broadcasted_iota(jnp.int32, square, 1)
    column = jnp.sum(jnp.where(same, gain[...], 0.0), axis=1, keepdims=True)
    high = column.astype(BF16)
    rest = column - high.astype(F32)
    middle = rest.astype(BF16)
    low = (rest - middle.astype(F32)).astype(BF16)
    lane = lax.broadcasted_iota(jnp.int32, mine.shape, 1)
    first = SLOTS - 8
    acc = jnp.where(lane == first, high.astype(F32), acc)
    acc = jnp.where(lane == first + 1, middle.astype(F32), acc)
    mine[...] = jnp.where(lane == first + 2, low.astype(F32), acc)


def pick_other_kernel(tok_dev, core_ref, swapped, ids, mine, out):
    acc = pick(tok_dev, 1 - core_ref[0], swapped, ids[...], mine.shape[0])
    total = (acc + mine[...]).astype(BF16)
    for g in range(out.shape[0]):
        out[g] = total


def member_kernel(plane_ref, core_ref, gathered, swapped, low, high):
    blocks = gathered.shape[0]
    tokens = low.shape[0]
    core = core_ref[0]
    base = (2 * plane_ref[0] + core) * tokens
    token = (lax.broadcasted_iota(jnp.int32, (tokens, 128), 0) + base).astype(F32)
    expert = lax.broadcasted_iota(jnp.int32, (tokens, 128), 1)
    member = jnp.zeros((tokens, 128), F32)
    for source in range(2):
        for b in range(blocks):
            lists = (gathered, swapped)[source][b, HALF : HALF + 8, :].astype(F32)
            ids = lists[:4] * 64.0 + lists[4:]
            found = jnp.zeros((tokens, 128), F32)
            for k in range(4):
                found += jnp.where(token == ids[k : k + 1], 1.0, 0.0)
            count = jnp.sum(found, axis=1, keepdims=True)
            which = 2 * b + (core if source == 0 else 1 - core)
            member += jnp.where(expert == which, count, 0.0)
    triangle = (tokens, tokens)
    earlier = lax.broadcasted_iota(jnp.int32, triangle, 1) < lax.broadcasted_iota(
        jnp.int32, triangle, 0
    )
    rank = jnp.dot(
        jnp.where(earlier, 1.0, 0.0).astype(BF16), member.astype(BF16), preferred_element_type=F32
    )
    slot = jnp.where(member > 0.5, rank, 255.0).astype(BF16)
    spread = (128, low.shape[1])
    line = lax.broadcasted_iota(jnp.int32, spread, 0) * SIDE
    place = lax.broadcasted_iota(jnp.int32, spread, 1)
    inside = (place >= line) & (place < line + SIDE)
    slots = jnp.dot(slot, jnp.where(inside, 1.0, 0.0).astype(BF16), preferred_element_type=F32)
    start = jnp.zeros(spread, jnp.int32) + jnp.where(inside, place - line, 0)
    start = jnp.sum(start.astype(F32), axis=0, keepdims=True)
    low[...] = jnp.where(slots == start, 1.0, 0.0).astype(BF16)
    high[...] = jnp.where(slots == start + float(SIDE), 1.0, 0.0).astype(BF16)


def block_of(core, corner, cell, ny, nx):
    Y, X = cell // (nx // 2), cell % (nx // 2)
    b, a = corner // 2, corner % 2
    return place(core, 2 * Y + b, 2 * X + a, ny, nx)


def turn_kernel(ny, nx, core_ref, gate_ref, up_ref, out):
    _, _, hid = gate_ref.shape
    cells = ny * nx // 4
    for s in range(4):
        for half, ref in enumerate((gate_ref, up_ref)):
            pieces = [ref[block_of(core_ref[0], s, g, ny, nx)] for g in range(cells)]
            rows = jnp.concatenate(pieces, axis=0)
            out[s, half * hid : (half + 1) * hid] = rows.T


def turn_down_kernel(ny, nx, core_ref, corner_ref, down_ref, w0, w1, w2, w3, turned):
    tp, part, hid = turned.shape
    for y in range(ny):
        rows = down_ref[:, y * nx * part : (y + 1) * nx * part].T
        turned[y * nx : (y + 1) * nx] = rows.reshape(nx, part, hid)
    for flip, out in enumerate((w0, w1, w2, w3)):
        for g in range(tp // 4):
            block = block_of(core_ref[0], corner_ref[0] ^ flip, g, ny, nx)
            out[g * part : (g + 1) * part] = turned[block]


def copies_kernel(array, out):
    for k in range(out.shape[0]):
        out[k] = array[...]


def hidden_kernel(x_ref, w_ref, out, normed):
    corners, depth, slots = x_ref.shape
    hid = out.shape[1]
    width = corners * depth
    square = jnp.zeros((1, slots), F32)
    for s in range(corners):
        v = x_ref[s].astype(F32)
        square += jnp.sum(v * v, axis=0, keepdims=True)
    scale = lax.rsqrt(square / width + EPS)
    acc = jnp.zeros((2 * hid, slots), F32)
    for s in range(corners):
        v = x_ref[s]
        parts = v[:, slots - 128 :].astype(F32)
        lane = lax.broadcasted_iota(jnp.int32, parts.shape, 1)
        keep = (lane >= 120) & (lane < 123)
        gain = jnp.sum(jnp.where(keep, parts, 0.0), axis=1, keepdims=True)
        normed[...] = (v.astype(F32) * scale * gain).astype(BF16)
        acc += jnp.dot(w_ref[s], normed[...], preferred_element_type=F32)
    gate, up = acc[:hid], acc[hid:]
    value = (gate / (1.0 + jnp.exp(-gate)) * up).astype(BF16)
    for k in range(out.shape[0]):
        out[k] = value


def down_kernel(corner_ref, hidden, w0, w1, w2, w3, out):
    me = corner_ref[0]
    acc = jnp.zeros(out.shape, F32)
    for flip, w in enumerate((w0, w1, w2, w3)):
        acc += jnp.dot(w[...], hidden[me ^ flip], preferred_element_type=F32)
    out[...] = acc.astype(BF16)


def send_kernel(arrived, affinity, low, high, out, weight):
    weight[...] = jnp.zeros(weight.shape, F32)
    weight[:, : affinity.shape[1]] = affinity[...]
    total = arrived[0].astype(F32)
    for g in range(1, arrived.shape[0]):
        total += arrived[g].astype(F32)
    weighted = (total * weight[...]).astype(BF16)
    empty = jnp.zeros_like(weighted)
    dims = (((1,), (1,)), ((), ()))
    rows = lax.dot_general(
        low[...],
        jnp.concatenate([weighted, empty], axis=0),
        dims,
        preferred_element_type=F32,
    )
    rows += lax.dot_general(
        high[...],
        jnp.concatenate([empty, weighted], axis=0),
        dims,
        preferred_element_type=F32,
    )
    out[...] = rows.astype(BF16)


def final_kernel(arrived, low, high, out):
    part = out.shape[0]
    total = jnp.dot(low[...], arrived[...], preferred_element_type=F32)[:, :part]
    total += jnp.dot(high[...], arrived[...], preferred_element_type=F32)[:, part:]
    out[...] = total.T.astype(BF16)


def local(tokens, norm_gain, chosen, affinity, w_gate, w_up, w_down):
    tok_dev, part = tokens.shape
    nz, ny, nx = lax.axis_size("z"), lax.axis_size("y"), lax.axis_size("x")
    experts = 2 * nz
    width, hid = w_gate.shape[1:]
    tp, cells = ny * nx, ny * nx // 4
    near, far = tiles(ny, nx)
    swap = [(0, 1), (1, 0)]
    core_index = lax.axis_index("core").astype(jnp.int32)
    z_index = lax.axis_index("z").astype(jnp.int32)
    y_index = lax.axis_index("y").astype(jnp.int32)
    x_index = lax.axis_index("x").astype(jnp.int32)
    corner_index = ((y_index + core_index) & 1) * 2 + ((x_index + core_index) & 1)
    core, corner = core_index.reshape(1), corner_index.reshape(1)
    plane = z_index.reshape(1)

    packed, own_ids = call(
        pack_kernel,
        [
            jax.ShapeDtypeStruct((nz, HALF + 8, 128), BF16),
            jax.ShapeDtypeStruct((1, SLOTS), jnp.int32),
        ],
        (tokens.T, chosen),
    )
    gathered = lax.all_to_all(packed, "z", 0, 0, tiled=True)

    down_shape = jax.ShapeDtypeStruct((cells * part, hid), BF16)
    downs = list(call(
        functools.partial(turn_down_kernel, ny, nx),
        [down_shape] * 4,
        (core, corner, w_down[0]),
        [SMEM, SMEM, VMEM],
        [pltpu.VMEM((tp, part, hid), BF16)],
        flops=1 << 30,
    ))
    for flip in range(1, 4):
        pairs = [(g[s], g[s ^ flip]) for g in near for s in range(4)]
        downs[flip] = lax.ppermute(downs[flip], PLANE, pairs)
    turned = call(
        functools.partial(turn_kernel, ny, nx),
        jax.ShapeDtypeStruct((4, 2 * hid, cells * part), BF16),
        (core, w_gate[0].reshape(tp, part, hid), w_up[0].reshape(tp, part, hid)),
        [SMEM, VMEM, VMEM],
        flops=1 << 30,
    )
    gathered, turned = lax.optimization_barrier((gathered, turned))

    swapped = lax.ppermute(gathered, "core", swap)
    own = call(
        functools.partial(pick_kernel, tok_dev),
        jax.ShapeDtypeStruct((part, SLOTS), F32),
        (core, gathered, own_ids, norm_gain[None]),
        [SMEM] + [VMEM] * 3,
        flops=2 * part * nz * tok_dev * SLOTS,
    )
    picked = call(
        functools.partial(pick_other_kernel, tok_dev),
        jax.ShapeDtypeStruct((cells, part, SLOTS), BF16),
        (core, swapped, own_ids, own),
        [SMEM] + [VMEM] * 3,
        flops=2 * part * nz * tok_dev * SLOTS,
    )

    column = lax.all_to_all(
        picked, PLANE, 0, 0, axis_index_groups=far, tiled=True
    ).reshape(cells * part, SLOTS)
    column, downs = lax.optimization_barrier((column, downs))
    copies = call(
        copies_kernel,
        jax.ShapeDtypeStruct((4, cells * part, SLOTS), BF16),
        (column,),
        flops=1 << 20,
    )
    full = lax.all_to_all(copies, PLANE, 0, 0, axis_index_groups=near, tiled=True)
    hidden = call(
        hidden_kernel,
        jax.ShapeDtypeStruct((4, hid, SLOTS), BF16),
        (full, turned),
        scratch=[pltpu.VMEM((cells * part, SLOTS), BF16)],
        flops=4 * width * hid * SLOTS,
    )
    tile_hidden = lax.all_to_all(hidden, PLANE, 0, 0, axis_index_groups=near, tiled=True)
    partial = call(
        down_kernel,
        jax.ShapeDtypeStruct((cells * part, SLOTS), BF16),
        (corner, tile_hidden, *downs),
        [SMEM] + [VMEM] * 5,
        flops=2 * width * hid * SLOTS,
    )
    late = lax.optimization_barrier((partial, own_ids, gathered, swapped))
    partial, own_ids, gathered, swapped = late
    arrived = lax.all_to_all(
        partial.reshape(cells, part, SLOTS), PLANE, 0, 0, axis_index_groups=far, tiled=True
    )
    hot_shape = jax.ShapeDtypeStruct((experts, SIDE, SLOTS), BF16)
    send_hot = call(
        functools.partial(send_hot_kernel, tok_dev),
        [hot_shape, hot_shape],
        (own_ids,),
        flops=1 << 30,
    )
    send_hot = [v.reshape(experts * SIDE, SLOTS) for v in send_hot]
    hot_shape = jax.ShapeDtypeStruct((tok_dev, experts * SIDE), BF16)
    final_hot = call(
        member_kernel,
        [hot_shape, hot_shape],
        (plane, core, gathered, swapped),
        [SMEM, SMEM, VMEM, VMEM],
        flops=1 << 31,
    )
    sent = call(
        send_kernel,
        jax.ShapeDtypeStruct((experts * SIDE, 128), BF16),
        (arrived, affinity, *send_hot),
        scratch=[pltpu.VMEM((1, SLOTS), F32)],
        flops=4 * 128 * experts * SIDE * SLOTS,
    )
    back = lax.all_to_all(
        sent.reshape(experts, SIDE, 128), ("z", "core"), 0, 0, tiled=True
    ).reshape(experts * SIDE, 128)
    total = call(
        final_kernel,
        jax.ShapeDtypeStruct((part, tok_dev), BF16),
        (back, *final_hot),
        flops=4 * 128 * experts * SIDE * tok_dev,
    )
    return total.T


def solution(mesh):
    nz, ny, nx = 12, 8, 4
    fine = Mesh(mesh.devices.reshape(nz, 2, ny, nx), ("z", "core", "y", "x"))
    ep, tp = ("z", "core"), ("y", "x")
    in_specs = (
        P(ep, tp),
        P(tp),
        P(ep, None),
        P(ep, None),
        P(ep, None, tp),
        P(ep, None, tp),
        P(ep, tp, None),
    )

    return jax.shard_map(local, mesh=fine, in_specs=in_specs, out_specs=P(ep, tp), check_vma=False)
```

```python
import functools

import jax
import jax.numpy as jnp
from jax import lax
from jax.experimental import pallas as pl
from jax.experimental.pallas import tpu as pltpu
from jax.sharding import Mesh, PartitionSpec as P


EPS = 1e-06
SLOTS = 512
HALF = 88
SIDE = 24
VMEM = pl.BlockSpec(memory_space=pltpu.VMEM)
SMEM = pl.BlockSpec(memory_space=pltpu.SMEM)
BF16 = jnp.bfloat16
F32 = jnp.float32
PLANE = ("core", "y", "x")


def call(kernel, outs, args, specs=None, scratch=(), flops=0, vmem=16):
    return pl.pallas_call(
        kernel,
        out_shape=outs,
        in_specs=specs or [VMEM] * len(args),
        out_specs=jax.tree.map(lambda _: VMEM, outs),
        scratch_shapes=list(scratch),
        compiler_params=pltpu.CompilerParams(vmem_limit_bytes=vmem * 1024 * 1024),
        cost_estimate=pl.CostEstimate(flops=flops, bytes_accessed=0, transcendentals=0),
    )(*args)


def place(core, y, x, ny, nx):
    return ((y + core) % ny) * nx + (x + core) % nx


def tiles(ny, nx):
    near, far = [], []
    for c in range(2):
        base = c * ny * nx

        def at(Y, X, b, a, c=c, base=base):
            return base + place(c, 2 * Y + b, 2 * X + a, ny, nx)

        corners = [(b, a) for b in range(2) for a in range(2)]
        cells = [(Y, X) for Y in range(ny // 2) for X in range(nx // 2)]
        near += [[at(Y, X, b, a) for b, a in corners] for Y, X in cells]
        far += [[at(Y, X, b, a) for Y, X in cells] for b, a in corners]
    return near, far


def hot(ids, base, rows):
    row = lax.broadcasted_iota(jnp.int32, (rows, ids.shape[1]), 0)
    return jnp.where(row == ids - base, 1.0, 0.0).astype(BF16)


def pack_kernel(tokens_ref, chosen_ref, out, ids, tokens, chosen, sems):
    copies, part = out.shape[0], tokens.shape[0]
    loads = [
        pltpu.make_async_copy(tokens_ref, tokens, sems.at[0]),
        pltpu.make_async_copy(chosen_ref, chosen, sems.at[1]),
    ]
    for load in loads:
        load.start()
    for load in loads:
        load.wait()
    ids[...] = jnp.full(ids.shape, 4095, jnp.int32)
    ids[:, : chosen.shape[1]] = chosen[...]
    turned = tokens[...].astype(F32).T
    rest = turned.shape[0] - HALF
    upper = jnp.concatenate([turned[HALF:], jnp.zeros((HALF - rest, part), F32)], axis=0)
    rows = jnp.concatenate([turned[:HALF], upper], axis=1)
    high = (ids[...] >> 6).astype(F32)
    low = (ids[...] & 63).astype(F32)
    lists = [v[:, k : k + 128] for v in (high, low) for k in range(0, SLOTS, 128)]
    body = jnp.concatenate([rows, *lists], axis=0).astype(BF16)
    for k in range(copies):
        out[k] = body


def send_hot_kernel(tok_dev, ids, low, high):
    side = ids.shape[1]
    token = ids[...].astype(F32)
    owner = jnp.floor((token + 0.5) * (1.0 / tok_dev))
    column = jnp.broadcast_to(token, (128, side)).T[:, :1]
    column_owner = jnp.broadcast_to(owner, (128, side)).T[:, :1]
    before = (column < token) & (column_owner == owner)
    rank = jnp.sum(jnp.where(before, 1.0, 0.0), axis=0, keepdims=True)
    code = (owner * (2.0 * SIDE) + rank).astype(jnp.int32)
    row = lax.broadcasted_iota(jnp.int32, (SIDE, side), 0)
    for o in range(low.shape[0]):
        low[o] = jnp.where(code == row + 2 * SIDE * o, 1.0, 0.0).astype(BF16)
        high[o] = jnp.where(code == row + 2 * SIDE * o + SIDE, 1.0, 0.0).astype(BF16)


def pick(tok_dev, core, gathered, ids, part):
    dims = (((0,), (0,)), ((), ()))
    acc = jnp.zeros((part, SLOTS), F32)
    for b in range(gathered.shape[0]):
        for half in range(2):
            base = (2 * b + core) * tok_dev + half * HALF
            rows = gathered[b, :HALF, half * part : (half + 1) * part]
            acc += lax.dot_general(rows, hot(ids, base, HALF), dims, preferred_element_type=F32)
    return acc


def pick_kernel(tok_dev, core_ref, gathered, ids, gain, mine):
    part = gain.shape[1]
    acc = pick(tok_dev, core_ref[0], gathered, ids[...], part)
    square = (part, part)
    same = lax.broadcasted_iota(jnp.int32, square, 0) == lax.broadcasted_iota(jnp.int32, square, 1)
    column = jnp.sum(jnp.where(same, gain[...], 0.0), axis=1, keepdims=True)
    high = column.astype(BF16)
    rest = column - high.astype(F32)
    middle = rest.astype(BF16)
    low = (rest - middle.astype(F32)).astype(BF16)
    lane = lax.broadcasted_iota(jnp.int32, mine.shape, 1)
    first = SLOTS - 8
    acc = jnp.where(lane == first, high.astype(F32), acc)
    acc = jnp.where(lane == first + 1, middle.astype(F32), acc)
    mine[...] = jnp.where(lane == first + 2, low.astype(F32), acc)


def pick_other_kernel(tok_dev, core_ref, swapped, ids, mine, out):
    acc = pick(tok_dev, 1 - core_ref[0], swapped, ids[...], mine.shape[0])
    total = (acc + mine[...]).astype(BF16)
    for g in range(out.shape[0]):
        out[g] = total


def member_kernel(plane_ref, core_ref, gathered, swapped, low, high):
    blocks = gathered.shape[0]
    tokens = low.shape[0]
    core = core_ref[0]
    base = (2 * plane_ref[0] + core) * tokens
    token = (lax.broadcasted_iota(jnp.int32, (tokens, 128), 0) + base).astype(F32)
    expert = lax.broadcasted_iota(jnp.int32, (tokens, 128), 1)
    member = jnp.zeros((tokens, 128), F32)
    for source in range(2):
        for b in range(blocks):
            lists = (gathered, swapped)[source][b, HALF : HALF + 8, :].astype(F32)
            ids = lists[:4] * 64.0 + lists[4:]
            found = jnp.zeros((tokens, 128), F32)
            for k in range(4):
                found += jnp.where(token == ids[k : k + 1], 1.0, 0.0)
            count = jnp.sum(found, axis=1, keepdims=True)
            which = 2 * b + (core if source == 0 else 1 - core)
            member += jnp.where(expert == which, count, 0.0)
    triangle = (tokens, tokens)
    earlier = lax.broadcasted_iota(jnp.int32, triangle, 1) < lax.broadcasted_iota(
        jnp.int32, triangle, 0
    )
    rank = jnp.dot(
        jnp.where(earlier, 1.0, 0.0).astype(BF16), member.astype(BF16), preferred_element_type=F32
    )
    slot = jnp.where(member > 0.5, rank, 255.0).astype(BF16)
    spread = (128, low.shape[1])
    line = lax.broadcasted_iota(jnp.int32, spread, 0) * SIDE
    place = lax.broadcasted_iota(jnp.int32, spread, 1)
    inside = (place >= line) & (place < line + SIDE)
    slots = jnp.dot(slot, jnp.where(inside, 1.0, 0.0).astype(BF16), preferred_element_type=F32)
    start = jnp.zeros(spread, jnp.int32) + jnp.where(inside, place - line, 0)
    start = jnp.sum(start.astype(F32), axis=0, keepdims=True)
    low[...] = jnp.where(slots == start, 1.0, 0.0).astype(BF16)
    high[...] = jnp.where(slots == start + float(SIDE), 1.0, 0.0).astype(BF16)


def block_of(core, corner, cell, ny, nx):
    Y, X = cell // (nx // 2), cell % (nx // 2)
    b, a = corner // 2, corner % 2
    return place(core, 2 * Y + b, 2 * X + a, ny, nx)


def turn_down_kernel(ny, nx, core_ref, corner_ref, down_ref, w0, w1, w2, w3, turned):
    tp, part, hid = turned.shape
    for y in range(ny):
        rows = down_ref[:, y * nx * part : (y + 1) * nx * part].T
        turned[y * nx : (y + 1) * nx] = rows.reshape(nx, part, hid)
    for flip, out in enumerate((w0, w1, w2, w3)):
        for g in range(tp // 4):
            block = block_of(core_ref[0], corner_ref[0] ^ flip, g, ny, nx)
            out[g * part : (g + 1) * part] = turned[block]


def copies_kernel(array, out):
    for k in range(out.shape[0]):
        out[k] = array[...]


def hidden_kernel(ny, nx, core_ref, x_ref, gate_ref, up_ref, out, normed):
    corners, depth, slots = x_ref.shape
    hid = out.shape[1]
    width = corners * depth
    square = jnp.zeros((1, slots), F32)
    for s in range(corners):
        v = x_ref[s].astype(F32)
        square += jnp.sum(v * v, axis=0, keepdims=True)
    scale = lax.rsqrt(square / width + EPS)
    gate = jnp.zeros((hid, slots), F32)
    up = jnp.zeros((hid, slots), F32)
    dims = (((0,), (0,)), ((), ()))
    for s in range(corners):
        v = x_ref[s]
        parts = v[:, slots - 128 :].astype(F32)
        lane = lax.broadcasted_iota(jnp.int32, parts.shape, 1)
        keep = (lane >= 120) & (lane < 123)
        gain = jnp.sum(jnp.where(keep, parts, 0.0), axis=1, keepdims=True)
        normed[...] = (v.astype(F32) * scale * gain).astype(BF16)
        places = [block_of(core_ref[0], s, g, ny, nx) for g in range(ny * nx // 4)]
        rows = jnp.concatenate([gate_ref[p] for p in places], axis=0)
        gate += lax.dot_general(rows, normed[...], dims, preferred_element_type=F32)
        rows = jnp.concatenate([up_ref[p] for p in places], axis=0)
        up += lax.dot_general(rows, normed[...], dims, preferred_element_type=F32)
    value = (gate / (1.0 + jnp.exp(-gate)) * up).astype(BF16)
    for k in range(out.shape[0]):
        out[k] = value


def down_kernel(corner_ref, hidden, w0, w1, w2, w3, out):
    me = corner_ref[0]
    acc = jnp.zeros(out.shape, F32)
    for flip, w in enumerate((w0, w1, w2, w3)):
        acc += jnp.dot(w[...], hidden[me ^ flip], preferred_element_type=F32)
    out[...] = acc.astype(BF16)


def send_kernel(arrived, affinity, low, high, out, weight):
    weight[...] = jnp.zeros(weight.shape, F32)
    weight[:, : affinity.shape[1]] = affinity[...]
    total = arrived[0].astype(F32)
    for g in range(1, arrived.shape[0]):
        total += arrived[g].astype(F32)
    weighted = (total * weight[...]).astype(BF16)
    empty = jnp.zeros_like(weighted)
    dims = (((1,), (1,)), ((), ()))
    rows = lax.dot_general(
        low[...],
        jnp.concatenate([weighted, empty], axis=0),
        dims,
        preferred_element_type=F32,
    )
    rows += lax.dot_general(
        high[...],
        jnp.concatenate([empty, weighted], axis=0),
        dims,
        preferred_element_type=F32,
    )
    out[...] = rows.astype(BF16)


def final_kernel(arrived, low, high, out):
    part = out.shape[0]
    total = jnp.dot(low[...], arrived[...], preferred_element_type=F32)[:, :part]
    total += jnp.dot(high[...], arrived[...], preferred_element_type=F32)[:, part:]
    out[...] = total.T.astype(BF16)


def local(tokens, norm_gain, chosen, affinity, w_gate, w_up, w_down):
    tok_dev, part = tokens.shape
    nz, ny, nx = lax.axis_size("z"), lax.axis_size("y"), lax.axis_size("x")
    experts = 2 * nz
    width, hid = w_gate.shape[1:]
    tp, cells = ny * nx, ny * nx // 4
    near, far = tiles(ny, nx)
    swap = [(0, 1), (1, 0)]
    core_index = lax.axis_index("core").astype(jnp.int32)
    z_index = lax.axis_index("z").astype(jnp.int32)
    y_index = lax.axis_index("y").astype(jnp.int32)
    x_index = lax.axis_index("x").astype(jnp.int32)
    corner_index = ((y_index + core_index) & 1) * 2 + ((x_index + core_index) & 1)
    core, corner = core_index.reshape(1), corner_index.reshape(1)
    plane = z_index.reshape(1)

    packed, own_ids = call(
        pack_kernel,
        [
            jax.ShapeDtypeStruct((nz, HALF + 8, 128), BF16),
            jax.ShapeDtypeStruct((1, SLOTS), jnp.int32),
        ],
        (tokens.T, chosen),
        [pl.BlockSpec(memory_space=pltpu.HBM)] * 2,
        [
            pltpu.VMEM((part, tok_dev), BF16),
            pltpu.VMEM(chosen.shape, jnp.int32),
            pltpu.SemaphoreType.DMA((2,)),
        ],
    )
    gathered = lax.all_to_all(packed, "z", 0, 0, tiled=True)

    down_shape = jax.ShapeDtypeStruct((cells * part, hid), BF16)
    downs = list(call(
        functools.partial(turn_down_kernel, ny, nx),
        [down_shape] * 4,
        (core, corner, w_down[0]),
        [SMEM, SMEM, VMEM],
        [pltpu.VMEM((tp, part, hid), BF16)],
        flops=1 << 30,
    ))
    for flip in range(1, 4):
        pairs = [(g[s], g[s ^ flip]) for g in near for s in range(4)]
        downs[flip] = lax.ppermute(downs[flip], PLANE, pairs)
    swapped = lax.ppermute(gathered, "core", swap)
    own = call(
        functools.partial(pick_kernel, tok_dev),
        jax.ShapeDtypeStruct((part, SLOTS), F32),
        (core, gathered, own_ids, norm_gain[None]),
        [SMEM] + [VMEM] * 3,
        flops=2 * part * nz * tok_dev * SLOTS,
    )
    swapped, downs = lax.optimization_barrier((swapped, downs))
    picked = call(
        functools.partial(pick_other_kernel, tok_dev),
        jax.ShapeDtypeStruct((cells, part, SLOTS), BF16),
        (core, swapped, own_ids, own),
        [SMEM] + [VMEM] * 3,
        flops=2 * part * nz * tok_dev * SLOTS,
    )

    column = lax.all_to_all(
        picked, PLANE, 0, 0, axis_index_groups=far, tiled=True
    ).reshape(cells * part, SLOTS)
    copies = call(
        copies_kernel,
        jax.ShapeDtypeStruct((4, cells * part, SLOTS), BF16),
        (column,),
        flops=1 << 20,
    )
    full = lax.all_to_all(copies, PLANE, 0, 0, axis_index_groups=near, tiled=True)
    hidden = call(
        functools.partial(hidden_kernel, ny, nx),
        jax.ShapeDtypeStruct((4, hid, SLOTS), BF16),
        (core, full, w_gate[0].reshape(tp, part, hid), w_up[0].reshape(tp, part, hid)),
        [SMEM] + [VMEM] * 3,
        scratch=[pltpu.VMEM((cells * part, SLOTS), BF16)],
        flops=4 * width * hid * SLOTS,
    )
    tile_hidden = lax.all_to_all(hidden, PLANE, 0, 0, axis_index_groups=near, tiled=True)
    partial = call(
        down_kernel,
        jax.ShapeDtypeStruct((cells * part, SLOTS), BF16),
        (corner, tile_hidden, *downs),
        [SMEM] + [VMEM] * 5,
        flops=2 * width * hid * SLOTS,
    )
    late = lax.optimization_barrier((partial, own_ids, gathered, swapped))
    partial, own_ids, gathered, swapped = late
    arrived = lax.all_to_all(
        partial.reshape(cells, part, SLOTS), PLANE, 0, 0, axis_index_groups=far, tiled=True
    )
    hot_shape = jax.ShapeDtypeStruct((experts, SIDE, SLOTS), BF16)
    send_hot = call(
        functools.partial(send_hot_kernel, tok_dev),
        [hot_shape, hot_shape],
        (own_ids,),
        flops=1 << 30,
    )
    send_hot = [v.reshape(experts * SIDE, SLOTS) for v in send_hot]
    hot_shape = jax.ShapeDtypeStruct((tok_dev, experts * SIDE), BF16)
    final_hot = call(
        member_kernel,
        [hot_shape, hot_shape],
        (plane, core, gathered, swapped),
        [SMEM, SMEM, VMEM, VMEM],
        flops=1 << 31,
    )
    sent = call(
        send_kernel,
        jax.ShapeDtypeStruct((experts * SIDE, 128), BF16),
        (arrived, affinity, *send_hot),
        scratch=[pltpu.VMEM((1, SLOTS), F32)],
        flops=4 * 128 * experts * SIDE * SLOTS,
    )
    back = lax.all_to_all(
        sent.reshape(experts, SIDE, 128), ("z", "core"), 0, 0, tiled=True
    ).reshape(experts * SIDE, 128)
    total = call(
        final_kernel,
        jax.ShapeDtypeStruct((part, tok_dev), BF16),
        (back, *final_hot),
        flops=4 * 128 * experts * SIDE * tok_dev,
    )
    return total.T


def solution(mesh):
    nz, ny, nx = 12, 8, 4
    fine = Mesh(mesh.devices.reshape(nz, 2, ny, nx), ("z", "core", "y", "x"))
    ep, tp = ("z", "core"), ("y", "x")
    in_specs = (
        P(ep, tp),
        P(tp),
        P(ep, None),
        P(ep, None),
        P(ep, None, tp),
        P(ep, None, tp),
        P(ep, tp, None),
    )

    return jax.shard_map(local, mesh=fine, in_specs=in_specs, out_specs=P(ep, tp), check_vma=False)
```

```python
import functools

import jax
import jax.numpy as jnp
from jax import lax
from jax.experimental import pallas as pl
from jax.experimental.pallas import tpu as pltpu
from jax.sharding import Mesh, PartitionSpec as P


EPS = 1e-06
SLOTS = 512
HALF = 88
SIDE = 24
USED = 21
NONE = 255.0
VMEM = pl.BlockSpec(memory_space=pltpu.VMEM)
SMEM = pl.BlockSpec(memory_space=pltpu.SMEM)
BF16 = jnp.bfloat16
F32 = jnp.float32
PLANE = ("core", "y", "x")


def call(kernel, outs, args, specs=None, scratch=(), flops=0, vmem=16):
    return pl.pallas_call(
        kernel,
        out_shape=outs,
        in_specs=specs or [VMEM] * len(args),
        out_specs=jax.tree.map(lambda _: VMEM, outs),
        scratch_shapes=list(scratch),
        compiler_params=pltpu.CompilerParams(vmem_limit_bytes=vmem * 1024 * 1024),
        cost_estimate=pl.CostEstimate(flops=flops, bytes_accessed=0, transcendentals=0),
    )(*args)


def place(core, y, x, ny, nx):
    return ((y + core) % ny) * nx + (x + core) % nx


def tiles(ny, nx):
    near, far = [], []
    for c in range(2):
        base = c * ny * nx

        def at(Y, X, b, a, c=c, base=base):
            return base + place(c, 2 * Y + b, 2 * X + a, ny, nx)

        corners = [(b, a) for b in range(2) for a in range(2)]
        cells = [(Y, X) for Y in range(ny // 2) for X in range(nx // 2)]
        near += [[at(Y, X, b, a) for b, a in corners] for Y, X in cells]
        far += [[at(Y, X, b, a) for Y, X in cells] for b, a in corners]
    return near, far


def hot(ids, base, rows):
    row = lax.broadcasted_iota(jnp.int32, (rows, ids.shape[1]), 0)
    return jnp.where(row == ids - base, 1.0, 0.0).astype(BF16)


def pack_kernel(tokens, out):
    copies, part = out.shape[0], tokens.shape[0]
    turned = tokens[...].astype(F32).T
    rest = turned.shape[0] - HALF
    upper = jnp.concatenate([turned[HALF:], jnp.zeros((HALF - rest, part), F32)], axis=0)
    rows = jnp.concatenate([turned[:HALF], upper], axis=1)
    body = rows.astype(BF16)
    for k in range(copies):
        out[k] = body


def send_hot_kernel(tok_dev, chosen, ids, low, high, extra):
    side = ids.shape[1]
    ids[...] = jnp.full(ids.shape, 4095, jnp.int32)
    ids[:, : chosen.shape[1]] = chosen[...]
    token = ids[...].astype(F32)
    owner = jnp.floor((token + 0.5) * (1.0 / tok_dev))
    local = token - owner * tok_dev
    column = jnp.broadcast_to(token, (128, side)).T[:, :1]
    column_owner = jnp.broadcast_to(owner, (128, side)).T[:, :1]
    before = (column < token) & (column_owner == owner)
    rank = jnp.sum(jnp.where(before, 1.0, 0.0), axis=0, keepdims=True)
    code = (owner * (2.0 * USED) + rank).astype(jnp.int32)
    row = lax.broadcasted_iota(jnp.int32, (SIDE, side), 0)
    slot = lax.broadcasted_iota(jnp.int32, (SIDE, 128), 0)
    lane = lax.broadcasted_iota(jnp.int32, (SIDE, 128), 1)
    for o in range(low.shape[0]):
        named = jnp.zeros((SIDE, 128), F32)
        for half, ref in enumerate((low, high)):
            match = (code == row + (2 * o + half) * USED) & (row < USED)
            ref[o] = jnp.where(match, 1.0, 0.0).astype(BF16)
            name = jnp.sum(jnp.where(match, local - NONE, 0.0), axis=1, keepdims=True)
            line = jnp.sum(jnp.where(slot == lane, name, 0.0), axis=0, keepdims=True) + NONE
            named = jnp.where(slot == USED + half, line, named)
        extra[o] = named


def pick(tok_dev, core, gathered, ids, part):
    dims = (((0,), (0,)), ((), ()))
    acc = jnp.zeros((part, SLOTS), F32)
    for b in range(gathered.shape[0]):
        for half in range(2):
            base = (2 * b + core) * tok_dev + half * HALF
            rows = gathered[b, :HALF, half * part : (half + 1) * part]
            acc += lax.dot_general(rows, hot(ids, base, HALF), dims, preferred_element_type=F32)
    return acc


def pick_kernel(tok_dev, core_ref, gathered, ids, gain, mine):
    part = gain.shape[1]
    acc = pick(tok_dev, core_ref[0], gathered, ids[...], part)
    square = (part, part)
    same = lax.broadcasted_iota(jnp.int32, square, 0) == lax.broadcasted_iota(jnp.int32, square, 1)
    column = jnp.sum(jnp.where(same, gain[...], 0.0), axis=1, keepdims=True)
    high = column.astype(BF16)
    rest = column - high.astype(F32)
    middle = rest.astype(BF16)
    low = (rest - middle.astype(F32)).astype(BF16)
    lane = lax.broadcasted_iota(jnp.int32, mine.shape, 1)
    first = SLOTS - 8
    acc = jnp.where(lane == first, high.astype(F32), acc)
    acc = jnp.where(lane == first + 1, middle.astype(F32), acc)
    mine[...] = jnp.where(lane == first + 2, low.astype(F32), acc)


def pick_other_kernel(tok_dev, core_ref, swapped, ids, mine, out):
    acc = pick(tok_dev, 1 - core_ref[0], swapped, ids[...], mine.shape[0])
    total = (acc + mine[...]).astype(BF16)
    for g in range(out.shape[0]):
        out[g] = total


def block_of(core, corner, cell, ny, nx):
    Y, X = cell // (nx // 2), cell % (nx // 2)
    b, a = corner // 2, corner % 2
    return place(core, 2 * Y + b, 2 * X + a, ny, nx)


def turn_down_kernel(ny, nx, core_ref, corner_ref, down_ref, w0, w1, w2, w3, turned):
    tp, part, hid = turned.shape
    for y in range(ny):
        rows = down_ref[:, y * nx * part : (y + 1) * nx * part].T
        turned[y * nx : (y + 1) * nx] = rows.reshape(nx, part, hid)
    for flip, out in enumerate((w0, w1, w2, w3)):
        for g in range(tp // 4):
            block = block_of(core_ref[0], corner_ref[0] ^ flip, g, ny, nx)
            out[g * part : (g + 1) * part] = turned[block]


def copies_kernel(array, out):
    for k in range(out.shape[0]):
        out[k] = array[...]


def hidden_kernel(ny, nx, core_ref, x_ref, gate_ref, up_ref, out, normed):
    corners, depth, slots = x_ref.shape
    hid = out.shape[1]
    width = corners * depth
    square = jnp.zeros((1, slots), F32)
    for s in range(corners):
        v = x_ref[s].astype(F32)
        square += jnp.sum(v * v, axis=0, keepdims=True)
    scale = lax.rsqrt(square / width + EPS)
    gate = jnp.zeros((hid, slots), F32)
    up = jnp.zeros((hid, slots), F32)
    dims = (((0,), (0,)), ((), ()))
    for s in range(corners):
        v = x_ref[s]
        parts = v[:, slots - 128 :].astype(F32)
        lane = lax.broadcasted_iota(jnp.int32, parts.shape, 1)
        keep = (lane >= 120) & (lane < 123)
        gain = jnp.sum(jnp.where(keep, parts, 0.0), axis=1, keepdims=True)
        normed[...] = (v.astype(F32) * scale * gain).astype(BF16)
        places = [block_of(core_ref[0], s, g, ny, nx) for g in range(ny * nx // 4)]
        rows = jnp.concatenate([gate_ref[p] for p in places], axis=0)
        gate += lax.dot_general(rows, normed[...], dims, preferred_element_type=F32)
        rows = jnp.concatenate([up_ref[p] for p in places], axis=0)
        up += lax.dot_general(rows, normed[...], dims, preferred_element_type=F32)
    value = (gate / (1.0 + jnp.exp(-gate)) * up).astype(BF16)
    for k in range(out.shape[0]):
        out[k] = value


def down_kernel(corner_ref, hidden, w0, w1, w2, w3, out):
    me = corner_ref[0]
    acc = jnp.zeros(out.shape, F32)
    for flip, w in enumerate((w0, w1, w2, w3)):
        acc += jnp.dot(w[...], hidden[me ^ flip], preferred_element_type=F32)
    out[...] = acc.astype(BF16)


def send_kernel(arrived, affinity, low, high, extra, out, weight):
    weight[...] = jnp.zeros(weight.shape, F32)
    weight[:, : affinity.shape[1]] = affinity[...]
    total = arrived[0].astype(F32)
    for g in range(1, arrived.shape[0]):
        total += arrived[g].astype(F32)
    weighted = (total * weight[...]).astype(BF16)
    empty = jnp.zeros_like(weighted)
    dims = (((1,), (1,)), ((), ()))
    rows = lax.dot_general(
        low[...],
        jnp.concatenate([weighted, empty], axis=0),
        dims,
        preferred_element_type=F32,
    )
    rows += lax.dot_general(
        high[...],
        jnp.concatenate([empty, weighted], axis=0),
        dims,
        preferred_element_type=F32,
    )
    out[...] = (rows + extra[...]).astype(BF16)


def final_kernel(arrived, out):
    part, tokens = out.shape
    experts = arrived.shape[0]
    slot = lax.broadcasted_iota(jnp.int32, (SIDE, 128), 0)
    lane = lax.broadcasted_iota(jnp.int32, (SIDE, 128), 1)
    token = lax.broadcasted_iota(jnp.int32, (SIDE, tokens), 1).astype(F32)
    hots = ([], [])
    for e in range(experts):
        block = arrived[e].astype(F32)
        for half in range(2):
            line = block[USED + half : USED + half + 1]
            name = jnp.sum(jnp.where(slot == lane, line, 0.0), axis=1, keepdims=True)
            hots[half].append(jnp.where(token == name, 1.0, 0.0))
    rows = arrived[...].reshape(experts * SIDE, 128)
    dims = (((0,), (0,)), ((), ()))
    low, high = (jnp.concatenate(h, axis=0).astype(BF16) for h in hots)
    total = lax.dot_general(rows, low, dims, preferred_element_type=F32)[:part]
    total += lax.dot_general(rows, high, dims, preferred_element_type=F32)[part:]
    out[...] = total.astype(BF16)


def local(tokens, norm_gain, chosen, affinity, w_gate, w_up, w_down):
    tok_dev, part = tokens.shape
    nz, ny, nx = lax.axis_size("z"), lax.axis_size("y"), lax.axis_size("x")
    experts = 2 * nz
    width, hid = w_gate.shape[1:]
    tp, cells = ny * nx, ny * nx // 4
    near, far = tiles(ny, nx)
    swap = [(0, 1), (1, 0)]
    core_index = lax.axis_index("core").astype(jnp.int32)
    y_index = lax.axis_index("y").astype(jnp.int32)
    x_index = lax.axis_index("x").astype(jnp.int32)
    corner_index = ((y_index + core_index) & 1) * 2 + ((x_index + core_index) & 1)
    core, corner = core_index.reshape(1), corner_index.reshape(1)

    packed = call(
        pack_kernel,
        jax.ShapeDtypeStruct((nz, HALF, 128), BF16),
        (tokens.T,),
    )
    gathered = lax.all_to_all(packed, "z", 0, 0, tiled=True)

    down_shape = jax.ShapeDtypeStruct((cells * part, hid), BF16)
    downs = list(call(
        functools.partial(turn_down_kernel, ny, nx),
        [down_shape] * 4,
        (core, corner, w_down[0]),
        [SMEM, SMEM, VMEM],
        [pltpu.VMEM((tp, part, hid), BF16)],
        flops=1 << 30,
    ))
    for flip in range(1, 4):
        pairs = [(g[s], g[s ^ flip]) for g in near for s in range(4)]
        downs[flip] = lax.ppermute(downs[flip], PLANE, pairs)
    hot_shape = jax.ShapeDtypeStruct((experts, SIDE, SLOTS), BF16)
    own_ids, *send_hot = call(
        functools.partial(send_hot_kernel, tok_dev),
        [
            jax.ShapeDtypeStruct((1, SLOTS), jnp.int32),
            hot_shape,
            hot_shape,
            jax.ShapeDtypeStruct((experts, SIDE, 128), F32),
        ],
        (chosen,),
        flops=1 << 30,
    )
    send_hot = [v.reshape(experts * SIDE, -1) for v in send_hot]
    swapped = lax.ppermute(gathered, "core", swap)
    own = call(
        functools.partial(pick_kernel, tok_dev),
        jax.ShapeDtypeStruct((part, SLOTS), F32),
        (core, gathered, own_ids, norm_gain[None]),
        [SMEM] + [VMEM] * 3,
        flops=2 * part * nz * tok_dev * SLOTS,
    )
    swapped, downs = lax.optimization_barrier((swapped, downs))
    picked = call(
        functools.partial(pick_other_kernel, tok_dev),
        jax.ShapeDtypeStruct((cells, part, SLOTS), BF16),
        (core, swapped, own_ids, own),
        [SMEM] + [VMEM] * 3,
        flops=2 * part * nz * tok_dev * SLOTS,
    )

    column = lax.all_to_all(
        picked, PLANE, 0, 0, axis_index_groups=far, tiled=True
    ).reshape(cells * part, SLOTS)
    copies = call(
        copies_kernel,
        jax.ShapeDtypeStruct((4, cells * part, SLOTS), BF16),
        (column,),
        flops=1 << 20,
    )
    full = lax.all_to_all(copies, PLANE, 0, 0, axis_index_groups=near, tiled=True)
    hidden = call(
        functools.partial(hidden_kernel, ny, nx),
        jax.ShapeDtypeStruct((4, hid, SLOTS), BF16),
        (core, full, w_gate[0].reshape(tp, part, hid), w_up[0].reshape(tp, part, hid)),
        [SMEM] + [VMEM] * 3,
        scratch=[pltpu.VMEM((cells * part, SLOTS), BF16)],
        flops=4 * width * hid * SLOTS,
    )
    tile_hidden = lax.all_to_all(hidden, PLANE, 0, 0, axis_index_groups=near, tiled=True)
    partial = call(
        down_kernel,
        jax.ShapeDtypeStruct((cells * part, SLOTS), BF16),
        (corner, tile_hidden, *downs),
        [SMEM] + [VMEM] * 5,
        flops=2 * width * hid * SLOTS,
    )
    arrived = lax.all_to_all(
        partial.reshape(cells, part, SLOTS), PLANE, 0, 0, axis_index_groups=far, tiled=True
    )
    sent = call(
        send_kernel,
        jax.ShapeDtypeStruct((experts * SIDE, 128), BF16),
        (arrived, affinity, *send_hot),
        scratch=[pltpu.VMEM((1, SLOTS), F32)],
        flops=4 * 128 * experts * SIDE * SLOTS,
    )
    back = lax.all_to_all(sent.reshape(experts, SIDE, 128), ("z", "core"), 0, 0, tiled=True)
    total = call(
        final_kernel,
        jax.ShapeDtypeStruct((part, tok_dev), BF16),
        (back,),
        flops=4 * 128 * experts * SIDE * tok_dev,
    )
    return total.T


def solution(mesh):
    nz, ny, nx = 12, 8, 4
    fine = Mesh(mesh.devices.reshape(nz, 2, ny, nx), ("z", "core", "y", "x"))
    ep, tp = ("z", "core"), ("y", "x")
    in_specs = (
        P(ep, tp),
        P(tp),
        P(ep, None),
        P(ep, None),
        P(ep, None, tp),
        P(ep, None, tp),
        P(ep, tp, None),
    )

    return jax.shard_map(local, mesh=fine, in_specs=in_specs, out_specs=P(ep, tp), check_vma=False)
```
